32 devices in a mesh: sp: 8 (over z, y), tp: 4 (over x, core).
Axes of the slice: x: 2, y: 2, z: 4, core: 2. Of those that a mesh axis runs over, the one named last changes fastest.
Arguments:
- prompt_input: bfloat16 [2304, 2048], P('sp'), may hold values from -6 to 6
- next_input: bfloat16 [2048], replicated, may hold values from -6 to 6
- norm_gain: float32 [2048], replicated, may hold values from 0.1 to 1.9
- w_key: bfloat16 [2048, 1024], P(None, 'tp'), may hold values from -0.125 to 0.125
- w_value: bfloat16 [2048, 1024], P(None, 'tp'), may hold values from -0.125 to 0.125
- w_query: bfloat16 [2048, 1024], P(None, 'tp'), may hold values from -0.125 to 0.125
- key_offset: float32 [2304, 8], P('sp', 'tp'), may hold values from -10 to 0, as said below
Outputs:
- key_cache: bfloat16 [8, 8, 36, 1024], P('sp', None, None, 'tp')
- value_cache: bfloat16 [8, 8, 36, 1024], P('sp', None, None, 'tp')
- reading: bfloat16 [1024], replicated
The draws below stay inside these ranges and needn't reach their ends.
Inputs may be any that keep to these rules, and one draw needn't show every extreme that they name: `key_offset`: finite log-odds offsets, one per key and head.
All inputs are finite; a program needn't handle non-finite values.
Results may differ from the reference program's by a relative error of at most 0.011.
Values may be sent and summed in bfloat16 or wider, within the bound.
A program may use at most 64 MiB of HBM per device.

```python
import math
import jax
import jax.numpy as jnp
from jax import lax

D = 2048
HEAD_COUNT = 8
HEAD_DIM = 128
SPAN = 288
PROMPT_LENGTH = 2304
SUB = 36
N_SP = 8


def draw_key_offset(key, part):
    head_order = jax.random.permutation(jax.random.fold_in(key, 11), HEAD_COUNT)
    fast_heads = head_order < HEAD_COUNT // 2
    slow_base = math.log(0.6 / PROMPT_LENGTH)
    fast_base = math.log(0.6 / 40.0)
    base_rate = jnp.where(fast_heads, fast_base, slow_base).astype(jnp.float32)
    block_shift = jax.random.uniform(jax.random.fold_in(key, 12), (HEAD_COUNT, PROMPT_LENGTH // SPAN), jnp.float32, -0.7, 0.7)
    block_shift = jnp.repeat(block_shift, SPAN, axis=1)
    rough_part = jax.random.uniform(jax.random.fold_in(key, 13), (HEAD_COUNT, PROMPT_LENGTH), jnp.float32, -1.0, 1.0)
    offset_table = base_rate[:, None] + block_shift + rough_part
    spike_position = jax.random.randint(jax.random.fold_in(key, 14), (HEAD_COUNT, 3), 0, PROMPT_LENGTH)
    position_slots = jnp.arange(PROMPT_LENGTH, dtype=jnp.int32)
    spike_matches = jnp.any(position_slots[None, None, :] == spike_position[..., None], axis=1)
    signal_level = jax.random.uniform(jax.random.fold_in(key, 15), (HEAD_COUNT, PROMPT_LENGTH), jnp.float32, -1.4, 0.0)
    gradual_mask = jnp.logical_not(fast_heads)[:, None]
    offset_table = jnp.where(jnp.logical_and(spike_matches, gradual_mask), signal_level, offset_table)
    offset_table = jnp.clip(offset_table, -10.0, 0.0)
    return jnp.transpose(offset_table, (1, 0)).astype(jnp.float32)


def steps_of(rng, shape, cuts, least, largest):
    level = 1.0
    for position, parts in cuts:
        steps = jax.random.uniform(jax.random.fold_in(jax.random.fold_in(rng, 6), position), (parts,), jnp.float32, least / len(cuts), largest / len(cuts))
        level = level * jnp.repeat(jnp.exp(steps), shape[position] // parts).reshape((-1,) + (1,) * (len(shape) - 1 - position))
    return level


def noise(key, extent, deviation, most, shards=(), held_as=jnp.bfloat16):
    drawn = deviation * jax.random.normal(key, extent, jnp.float32)
    if shards:
        drawn = drawn * steps_of(key, extent, shards, -0.22, 0.18)
    return jnp.clip(drawn, -most, most).astype(held_as)


def setup_inputs(seed: int = 0) -> dict:
    streams_of = jax.random.split(jax.random.key(seed), 8)
    return {
        "prompt_input": noise(streams_of[0], (PROMPT_LENGTH, D), 1.0, 6.0, ((0, 8),)),
        "next_input": noise(streams_of[1], (D,), 1.0, 6.0),
        "norm_gain": jnp.clip(1.0 + 0.18 * jax.random.normal(streams_of[2], (D,), jnp.float32), 0.1, 1.9),
        "w_key": noise(streams_of[3], (D, HEAD_COUNT * HEAD_DIM), D ** -0.5, 0.125, ((1, 4),)),
        "w_value": noise(streams_of[4], (D, HEAD_COUNT * HEAD_DIM), D ** -0.5, 0.125, ((1, 4),)),
        "w_query": noise(streams_of[5], (D, HEAD_COUNT * HEAD_DIM), D ** -0.5, 0.125, ((1, 4),)),
        "key_offset": draw_key_offset(jax.random.fold_in(streams_of[7], 71), 0),
    }


def norm_rows(row_block, gain_vec):
    wide_rows = row_block.astype(jnp.float32)
    inv_rms = lax.rsqrt(lax.optimization_barrier(jnp.mean(wide_rows * wide_rows, axis=-1, keepdims=True)) + 1e-06)
    return (wide_rows * inv_rms * gain_vec).astype(jnp.bfloat16)

def lay_out(cache_rows):
    blocks = cache_rows.reshape(N_SP, N_SP, SUB, HEAD_COUNT * HEAD_DIM)
    return jnp.transpose(blocks, (1, 0, 2, 3))

def reference(prompt_input, next_input, norm_gain, w_key, w_value, w_query, key_offset):
    normed = norm_rows(prompt_input, norm_gain)
    keys = jnp.dot(normed, w_key, preferred_element_type=jnp.float32).astype(jnp.bfloat16)
    values = jnp.dot(normed, w_value, preferred_element_type=jnp.float32).astype(jnp.bfloat16)
    query_normed = norm_rows(next_input[None, :], norm_gain)
    new_query = jnp.dot(query_normed, w_query, preferred_element_type=jnp.float32).astype(jnp.bfloat16)
    new_query = new_query.reshape(HEAD_COUNT, HEAD_DIM).astype(jnp.float32)
    key_heads = keys.reshape(PROMPT_LENGTH, HEAD_COUNT, HEAD_DIM).astype(jnp.float32)
    value_heads = values.reshape(PROMPT_LENGTH, HEAD_COUNT, HEAD_DIM).astype(jnp.float32)
    logits = jnp.einsum('hd,shd->sh', new_query, key_heads) * HEAD_DIM ** (-0.5) + key_offset
    log_breaks = jax.nn.log_sigmoid(-logits)
    later = lax.cumsum(log_breaks, axis=0, reverse=True) - log_breaks
    weights = jnp.exp(jax.nn.log_sigmoid(logits) + later)
    reading = jnp.einsum('sh,shd->hd', weights, value_heads)
    reading = reading.reshape(HEAD_COUNT * HEAD_DIM).astype(jnp.bfloat16)
    return (lay_out(keys), lay_out(values), reading)
```

```python
import functools

import jax
import jax.numpy as jnp
from jax import lax
from jax.experimental import pallas as pl
from jax.experimental.pallas import tpu as pltpu
from jax.sharding import PartitionSpec as P

HEAD_DIM = 128
MESH = pl.DeviceIdType.MESH


def norm_rows(rows, gain):
    wide = rows.astype(jnp.float32)
    inv_rms = lax.rsqrt(jnp.mean(wide * wide, axis=-1, keepdims=True) + 1e-06)
    return (wide * inv_rms * gain).astype(jnp.bfloat16)


def split_parts(wide, count):
    parts = []
    for _ in range(count):
        part = wide.astype(jnp.bfloat16).astype(jnp.float32)
        parts.append(part)
        wide = wide - part
    return jnp.concatenate(parts, axis=0).astype(jnp.bfloat16)


def fold_parts(rows, heads):
    total = rows[:heads]
    for first in range(heads, rows.shape[0], heads):
        total = total + rows[first : first + heads]
    return total


def kernel(
    n_sp, n_tp, chunks,
    x_hbm, next_hbm, gain_hbm, wk_hbm, wv_hbm, wq_hbm, offset_hbm,
    k_out, v_out, read_out,
    x_in, normed, next_in, gain_in, wk, wv, wq, offset,
    k_send, v_send, message, gathered, head_message, head_gathered,
    x_sem, load_sem, own_sem,
    k_ssem, k_rsem, v_ssem, v_rsem, m_ssem, m_rsem, h_ssem, h_rsem,
):
    me = lax.axis_index("sp")
    lane = lax.axis_index("tp")
    span, width = x_hbm.shape[0], wk_hbm.shape[1]
    heads = width // HEAD_DIM
    sub = span // n_sp
    rows = span // chunks

    loads = [
        pltpu.make_async_copy(hbm, vmem, load_sem.at[n])
        for n, (hbm, vmem) in enumerate(
            [
                (gain_hbm, gain_in),
                (wk_hbm, wk),
                (wv_hbm, wv),
                (next_hbm, next_in),
                (wq_hbm, wq),
                (offset_hbm, offset),
            ]
        )
    ]
    x_loads = [
        pltpu.make_async_copy(
            x_hbm.at[pl.ds(c * rows, rows)], x_in.at[pl.ds(c * rows, rows)], x_sem.at[c]
        )
        for c in range(chunks)
    ]
    loads[0].start()
    for load in x_loads:
        load.start()
    for load in loads[1:]:
        load.start()

    barrier = pltpu.get_barrier_semaphore()

    @pl.loop(1, n_sp)
    def _(step):
        pl.semaphore_signal(
            barrier, inc=1, device_id=(lax.rem(me + step, n_sp), lane), device_id_type=MESH
        )

    @pl.loop(1, n_tp)
    def _(step):
        pl.semaphore_signal(
            barrier, inc=1, device_id=(me, lax.rem(lane + step, n_tp)), device_id_type=MESH
        )

    loads[0].wait()
    gain = gain_in[...]
    step_rows = 16 if rows % 16 == 0 else rows
    for c in range(chunks):
        x_loads[c].wait()
        for first in range(c * rows, (c + 1) * rows, step_rows):
            normed[first : first + step_rows, :] = norm_rows(x_in[first : first + step_rows, :], gain)

    def copies(step, send, recv, ssem, rsem):
        to = lax.rem(me + step, n_sp)
        return pltpu.make_async_remote_copy(
            src_ref=send.at[to], dst_ref=recv.at[me],
            send_sem=ssem.at[step], recv_sem=rsem.at[step],
            device_id=(to, lane), device_id_type=MESH,
        )

    def project(weight, send):
        wide = jnp.dot(normed[...], weight[...], preferred_element_type=jnp.float32)
        for slot in range(n_sp):
            send[slot] = wide[slot * sub : (slot + 1) * sub].astype(jnp.bfloat16)
        return wide.astype(jnp.bfloat16)

    loads[1].wait()
    keys = project(wk, k_send)
    pl.semaphore_wait(barrier, n_sp + n_tp - 2)

    @pl.loop(1, n_sp)
    def _(step):
        copies(step, k_send, k_out, k_ssem, k_rsem).start()

    own_key = pltpu.make_async_copy(k_send.at[me], k_out.at[me], own_sem.at[0])
    own_key.start()

    loads[3].wait()
    loads[4].wait()
    loads[5].wait()
    query_normed = jnp.broadcast_to(norm_rows(next_in[...], gain), (16, x_hbm.shape[1]))
    query = jnp.dot(query_normed, wq[...], preferred_element_type=jnp.float32)
    row_ids = lax.broadcasted_iota(jnp.int32, query.shape, 0)
    head_ids = lax.broadcasted_iota(jnp.int32, query.shape, 1) // HEAD_DIM
    query = jnp.where(row_ids == head_ids, query, 0.0).astype(jnp.bfloat16)
    logits = lax.dot_general(
        query, keys, (((1,), (1,)), ((), ())), preferred_element_type=jnp.float32
    )[:heads]
    logits = logits * HEAD_DIM ** (-0.5) + offset[...]
    tail = jnp.log1p(jnp.exp(-jnp.abs(logits)))
    log_breaks = -jnp.maximum(logits, 0.0) - tail
    later_than = (
        lax.broadcasted_iota(jnp.int32, (span, span), 0)
        > lax.broadcasted_iota(jnp.int32, (span, span), 1)
    )
    later_than = jnp.where(later_than, 1.0, 0.0).astype(jnp.bfloat16)
    inner = fold_parts(
        jnp.dot(split_parts(log_breaks, 3), later_than, preferred_element_type=jnp.float32), heads
    )
    block_total = jnp.sum(log_breaks, axis=1, keepdims=True)
    weights = jnp.exp(jnp.minimum(logits, 0.0) - tail + inner)

    loads[2].wait()
    values = project(wv, v_send)
    read = fold_parts(
        jnp.dot(split_parts(weights, 2), values, preferred_element_type=jnp.float32), heads
    )
    for head in range(heads):
        message[head : head + 1, :] = read[head : head + 1, head * HEAD_DIM : (head + 1) * HEAD_DIM]
        message[heads + head : heads + head + 1, :] = jnp.broadcast_to(
            block_total[head : head + 1], (1, HEAD_DIM)
        )

    def message_copy(step):
        return pltpu.make_async_remote_copy(
            src_ref=message, dst_ref=gathered.at[me],
            send_sem=m_ssem.at[step], recv_sem=m_rsem.at[step],
            device_id=(lax.rem(me + step, n_sp), lane), device_id_type=MESH,
        )

    @pl.loop(1, n_sp)
    def _(step):
        message_copy(step).start()

    own_message = pltpu.make_async_copy(message, gathered.at[me], own_sem.at[2])
    own_message.start()

    @pl.loop(1, n_sp)
    def _(step):
        copies(step, v_send, v_out, v_ssem, v_rsem).start()

    own_value = pltpu.make_async_copy(v_send.at[me], v_out.at[me], own_sem.at[1])
    own_value.start()

    own_message.wait()

    @pl.loop(1, n_sp)
    def _(step):
        message_copy(step).wait_recv()

    def add_block(step, carry):
        total, carried = carry
        block = gathered[n_sp - 1 - step]
        total = total + jnp.exp(carried) * block[:heads]
        return total, carried + block[heads : 2 * heads]

    zero = jnp.zeros((heads, HEAD_DIM), jnp.float32)
    total, _ = lax.fori_loop(0, n_sp, add_block, (zero, zero), unroll=n_sp <= 16)
    head_message[:heads, :] = total

    def head_copy(step):
        return pltpu.make_async_remote_copy(
            src_ref=head_message, dst_ref=head_gathered.at[lane],
            send_sem=h_ssem.at[step], recv_sem=h_rsem.at[step],
            device_id=(me, lax.rem(lane + step, n_tp)), device_id_type=MESH,
        )

    @pl.loop(1, n_tp)
    def _(step):
        head_copy(step).start()

    own_head = pltpu.make_async_copy(head_message, head_gathered.at[lane], own_sem.at[3])
    own_head.start()
    own_head.wait()

    @pl.loop(1, n_tp)
    def _(step):
        head_copy(step).wait_recv()

    read_out[...] = jnp.concatenate(
        [head_gathered[part, :heads, :] for part in range(n_tp)], axis=0
    ).astype(jnp.bfloat16)

    own_key.wait()
    own_value.wait()

    @pl.loop(1, n_tp)
    def _(step):
        head_copy(step).wait_send()

    @pl.loop(1, n_sp)
    def _(step):
        message_copy(step).wait_send()
        copies(step, k_send, k_out, k_ssem, k_rsem).wait()
        copies(step, v_send, v_out, v_ssem, v_rsem).wait()


def shards(prompt_input, next_input, norm_gain, w_key, w_value, w_query, key_offset):
    span, depth = prompt_input.shape
    width = w_key.shape[1]
    heads = width // HEAD_DIM
    n_sp, n_tp = lax.axis_size("sp"), lax.axis_size("tp")
    sub = span // n_sp
    chunks = 3 if span % 48 == 0 else 1
    message_rows = -(-2 * heads // 8) * 8
    head_rows = -(-heads // 8) * 8
    wide, narrow = jnp.float32, jnp.bfloat16
    cache = jax.ShapeDtypeStruct((n_sp, sub, width), narrow)
    sems = pltpu.SemaphoreType.DMA
    key_cache, value_cache, reading = pl.pallas_call(
        functools.partial(kernel, n_sp, n_tp, chunks),
        out_shape=(cache, cache, jax.ShapeDtypeStruct((n_tp * heads, HEAD_DIM), narrow)),
        in_specs=[pl.BlockSpec(memory_space=pl.ANY)] * 7,
        out_specs=(pl.BlockSpec(memory_space=pltpu.VMEM),) * 3,
        scratch_shapes=[
            pltpu.VMEM((span, depth), narrow),
            pltpu.VMEM((span, depth), narrow),
            pltpu.VMEM((1, depth), wide),
            pltpu.VMEM((1, depth), wide),
            pltpu.VMEM((depth, width), narrow),
            pltpu.VMEM((depth, width), narrow),
            pltpu.VMEM((depth, width), narrow),
            pltpu.VMEM((heads, span), wide),
            pltpu.VMEM((n_sp, sub, width), narrow),
            pltpu.VMEM((n_sp, sub, width), narrow),
            pltpu.VMEM((message_rows, HEAD_DIM), wide),
            pltpu.VMEM((n_sp, message_rows, HEAD_DIM), wide),
            pltpu.VMEM((head_rows, HEAD_DIM), wide),
            pltpu.VMEM((n_tp, head_rows, HEAD_DIM), wide),
            sems((chunks,)),
            sems((6,)),
            sems((4,)),
            sems((n_sp,)),
            sems((n_sp,)),
            sems((n_sp,)),
            sems((n_sp,)),
            sems((n_sp,)),
            sems((n_sp,)),
            sems((n_tp,)),
            sems((n_tp,)),
        ],
        compiler_params=pltpu.CompilerParams(collective_id=0, has_side_effects=True),
        name="prefill",
    )(
        prompt_input,
        next_input.astype(wide)[None],
        norm_gain[None],
        w_key,
        w_value,
        w_query,
        key_offset.T,
    )
    return key_cache[None], value_cache[None], reading.reshape(-1)


def solution(mesh):
    placed = (P("sp", None), P(), P(), P(None, "tp"), P(None, "tp"), P(None, "tp"), P("sp", "tp"))
    return jax.shard_map(
        shards,
        mesh=mesh,
        in_specs=placed,
        out_specs=(P("sp", None, None, "tp"), P("sp", None, None, "tp"), P()),
        check_vma=False,
    )
```

```python
import functools

import jax
import jax.numpy as jnp
from jax import lax
from jax.experimental import pallas as pl
from jax.experimental.pallas import tpu as pltpu
from jax.sharding import PartitionSpec as P

HEAD_DIM = 128
MESH = pl.DeviceIdType.MESH


def norm_rows(rows, gain):
    wide = rows.astype(jnp.float32)
    inv_rms = lax.rsqrt(jnp.mean(wide * wide, axis=-1, keepdims=True) + 1e-06)
    return (wide * inv_rms * gain).astype(jnp.bfloat16)


def split_parts(wide, count):
    parts = []
    for _ in range(count):
        part = wide.astype(jnp.bfloat16).astype(jnp.float32)
        parts.append(part)
        wide = wide - part
    return jnp.concatenate(parts, axis=0).astype(jnp.bfloat16)


def fold_parts(rows, heads):
    total = rows[:heads]
    for first in range(heads, rows.shape[0], heads):
        total = total + rows[first : first + heads]
    return total


def kernel(
    n_sp, n_tp, chunks,
    x_hbm, next_hbm, gain_hbm, wk_hbm, wv_hbm, wq_hbm, offset_hbm,
    k_out, v_out, read_out,
    x_in, normed, next_in, gain_in, wk, wv, wq, offset,
    k_send, v_send, message, gathered, head_message, head_gathered,
    x_sem, load_sem, own_sem,
    k_ssem, k_rsem, v_ssem, v_rsem, m_ssem, m_rsem, h_ssem, h_rsem,
):
    me = lax.axis_index("sp")
    lane = lax.axis_index("tp")
    span, width = x_hbm.shape[0], wk_hbm.shape[1]
    heads = width // HEAD_DIM
    sub = span // n_sp
    rows = span // chunks

    loads = [
        pltpu.make_async_copy(hbm, vmem, load_sem.at[n])
        for n, (hbm, vmem) in enumerate(
            [
                (gain_hbm, gain_in),
                (wk_hbm, wk),
                (wv_hbm, wv),
                (next_hbm, next_in),
                (wq_hbm, wq),
                (offset_hbm, offset),
            ]
        )
    ]
    x_loads = [
        pltpu.make_async_copy(
            x_hbm.at[pl.ds(c * rows, rows)], x_in.at[pl.ds(c * rows, rows)], x_sem.at[c]
        )
        for c in range(chunks)
    ]
    loads[0].start()
    for load in x_loads:
        load.start()
    for load in loads[1:]:
        load.start()

    barrier = pltpu.get_barrier_semaphore()

    @pl.loop(1, n_sp)
    def _(step):
        pl.semaphore_signal(
            barrier, inc=1, device_id=(lax.rem(me + step, n_sp), lane), device_id_type=MESH
        )

    @pl.loop(1, n_tp)
    def _(step):
        pl.semaphore_signal(
            barrier, inc=1, device_id=(me, lax.rem(lane + step, n_tp)), device_id_type=MESH
        )

    loads[0].wait()
    gain = gain_in[...]
    step_rows = 16 if rows % 16 == 0 else rows
    for c in range(chunks):
        x_loads[c].wait()
        for first in range(c * rows, (c + 1) * rows, step_rows):
            normed[first : first + step_rows, :] = norm_rows(x_in[first : first + step_rows, :], gain)

    def copies(step, send, recv, ssem, rsem):
        to = lax.rem(me + step, n_sp)
        return pltpu.make_async_remote_copy(
            src_ref=send.at[to], dst_ref=recv.at[me],
            send_sem=ssem.at[step], recv_sem=rsem.at[step],
            device_id=(to, lane), device_id_type=MESH,
        )

    def project(weight, send):
        wide = jnp.dot(normed[...], weight[...], preferred_element_type=jnp.float32)
        for slot in range(n_sp):
            send[slot] = wide[slot * sub : (slot + 1) * sub].astype(jnp.bfloat16)
        return wide.astype(jnp.bfloat16)

    loads[1].wait()
    keys = project(wk, k_send)
    pl.semaphore_wait(barrier, n_sp + n_tp - 2)

    @pl.loop(1, n_sp)
    def _(step):
        copies(step, k_send, k_out, k_ssem, k_rsem).start()

    own_key = pltpu.make_async_copy(k_send.at[me], k_out.at[me], own_sem.at[0])
    own_key.start()

    loads[3].wait()
    loads[4].wait()
    loads[5].wait()
    next_row = next_in[...].astype(jnp.float32)
    next_row = jnp.concatenate([next_row[n : n + 1] for n in range(next_row.shape[0])], axis=1)
    query_normed = jnp.broadcast_to(norm_rows(next_row, gain), (16, x_hbm.shape[1]))
    query = jnp.dot(query_normed, wq[...], preferred_element_type=jnp.float32)
    row_ids = lax.broadcasted_iota(jnp.int32, query.shape, 0)
    head_ids = lax.broadcasted_iota(jnp.int32, query.shape, 1) // HEAD_DIM
    query = jnp.where(row_ids == head_ids, query, 0.0).astype(jnp.bfloat16)
    logits = lax.dot_general(
        query, keys, (((1,), (1,)), ((), ())), preferred_element_type=jnp.float32
    )[:heads]
    logits = logits * HEAD_DIM ** (-0.5) + offset[...]
    tail = jnp.log1p(jnp.exp(-jnp.abs(logits)))
    log_breaks = -jnp.maximum(logits, 0.0) - tail
    later_than = (
        lax.broadcasted_iota(jnp.int32, (span, span), 0)
        > lax.broadcasted_iota(jnp.int32, (span, span), 1)
    )
    later_than = jnp.where(later_than, 1.0, 0.0).astype(jnp.bfloat16)
    inner = fold_parts(
        jnp.dot(split_parts(log_breaks, 3), later_than, preferred_element_type=jnp.float32), heads
    )
    block_total = jnp.sum(log_breaks, axis=1, keepdims=True)
    weights = jnp.exp(jnp.minimum(logits, 0.0) - tail + inner)

    loads[2].wait()
    values = project(wv, v_send)
    read = fold_parts(
        jnp.dot(split_parts(weights, 2), values, preferred_element_type=jnp.float32), heads
    )
    for head in range(heads):
        message[head : head + 1, :] = read[head : head + 1, head * HEAD_DIM : (head + 1) * HEAD_DIM]
        message[heads + head : heads + head + 1, :] = jnp.broadcast_to(
            block_total[head : head + 1], (1, HEAD_DIM)
        )

    def message_copy(step):
        return pltpu.make_async_remote_copy(
            src_ref=message, dst_ref=gathered.at[me],
            send_sem=m_ssem.at[step], recv_sem=m_rsem.at[step],
            device_id=(lax.rem(me + step, n_sp), lane), device_id_type=MESH,
        )

    @pl.loop(1, n_sp)
    def _(step):
        message_copy(step).start()

    own_message = pltpu.make_async_copy(message, gathered.at[me], own_sem.at[2])
    own_message.start()

    @pl.loop(1, n_sp)
    def _(step):
        copies(step, v_send, v_out, v_ssem, v_rsem).start()

    own_value = pltpu.make_async_copy(v_send.at[me], v_out.at[me], own_sem.at[1])
    own_value.start()

    own_message.wait()

    @pl.loop(1, n_sp)
    def _(step):
        message_copy(step).wait_recv()

    def add_block(step, carry):
        total, carried = carry
        block = gathered[n_sp - 1 - step]
        total = total + jnp.exp(carried) * block[:heads]
        return total, carried + block[heads : 2 * heads]

    zero = jnp.zeros((heads, HEAD_DIM), jnp.float32)
    total, _ = lax.fori_loop(0, n_sp, add_block, (zero, zero), unroll=n_sp <= 16)
    head_message[:heads, :] = total

    def head_copy(step):
        return pltpu.make_async_remote_copy(
            src_ref=head_message, dst_ref=head_gathered.at[lane],
            send_sem=h_ssem.at[step], recv_sem=h_rsem.at[step],
            device_id=(me, lax.rem(lane + step, n_tp)), device_id_type=MESH,
        )

    @pl.loop(1, n_tp)
    def _(step):
        head_copy(step).start()

    own_head = pltpu.make_async_copy(head_message, head_gathered.at[lane], own_sem.at[3])
    own_head.start()
    own_head.wait()

    @pl.loop(1, n_tp)
    def _(step):
        head_copy(step).wait_recv()

    read_out[...] = jnp.concatenate(
        [head_gathered[part, :heads, :] for part in range(n_tp)], axis=0
    ).astype(jnp.bfloat16)

    own_key.wait()
    own_value.wait()

    @pl.loop(1, n_tp)
    def _(step):
        head_copy(step).wait_send()

    @pl.loop(1, n_sp)
    def _(step):
        message_copy(step).wait_send()
        copies(step, k_send, k_out, k_ssem, k_rsem).wait()
        copies(step, v_send, v_out, v_ssem, v_rsem).wait()


def finish(k_in, v_in, read_in, k_out, v_out, read_out):
    for landed, out in ((k_in, k_out), (v_in, v_out)):
        out[...] = jnp.swapaxes(landed[...].astype(jnp.float32), 0, 1).astype(jnp.bfloat16)
    read_out[...] = read_in[...]


def shards(prompt_input, next_input, norm_gain, w_key, w_value, w_query, key_offset):
    span, depth = prompt_input.shape
    width = w_key.shape[1]
    heads = width // HEAD_DIM
    n_sp, n_tp = lax.axis_size("sp"), lax.axis_size("tp")
    sub = span // n_sp
    chunks = 3 if span % 48 == 0 else 1
    message_rows = -(-2 * heads // 8) * 8
    head_rows = -(-heads // 8) * 8
    wide, narrow = jnp.float32, jnp.bfloat16
    cache = jax.ShapeDtypeStruct((n_sp, sub, width), narrow)
    sems = pltpu.SemaphoreType.DMA
    landed = pl.pallas_call(
        functools.partial(kernel, n_sp, n_tp, chunks),
        out_shape=(cache, cache, jax.ShapeDtypeStruct((n_tp * heads, HEAD_DIM), narrow)),
        in_specs=[pl.BlockSpec(memory_space=pltpu.HBM)] * 7,
        out_specs=(pl.BlockSpec(memory_space=pltpu.VMEM),) * 3,
        scratch_shapes=[
            pltpu.VMEM((span, depth), narrow),
            pltpu.VMEM((span, depth), narrow),
            pltpu.VMEM((depth // HEAD_DIM, HEAD_DIM), narrow),
            pltpu.VMEM((1, depth), wide),
            pltpu.VMEM((depth, width), narrow),
            pltpu.VMEM((depth, width), narrow),
            pltpu.VMEM((depth, width), narrow),
            pltpu.VMEM((heads, span), wide),
            pltpu.VMEM((n_sp, sub, width), narrow),
            pltpu.VMEM((n_sp, sub, width), narrow),
            pltpu.VMEM((message_rows, HEAD_DIM), wide),
            pltpu.VMEM((n_sp, message_rows, HEAD_DIM), wide),
            pltpu.VMEM((head_rows, HEAD_DIM), wide),
            pltpu.VMEM((n_tp, head_rows, HEAD_DIM), wide),
            sems((chunks,)),
            sems((6,)),
            sems((4,)),
            sems((n_sp,)),
            sems((n_sp,)),
            sems((n_sp,)),
            sems((n_sp,)),
            sems((n_sp,)),
            sems((n_sp,)),
            sems((n_tp,)),
            sems((n_tp,)),
        ],
        compiler_params=pltpu.CompilerParams(
            collective_id=0, has_side_effects=True, vmem_limit_bytes=16 * 2**20
        ),
        name="prefill",
    )(
        *[
            pltpu.with_memory_space_constraint(operand, pltpu.HBM)
            for operand in (
                prompt_input,
                next_input.reshape(-1, HEAD_DIM),
                norm_gain[None],
                w_key,
                w_value,
                w_query,
                key_offset.T,
            )
        ]
    )
    slotted = jax.ShapeDtypeStruct((sub, n_sp, width), narrow)
    key_cache, value_cache, reading = pl.pallas_call(
        finish,
        out_shape=(slotted, slotted, jax.ShapeDtypeStruct((n_tp * heads, HEAD_DIM), narrow)),
        in_specs=[pl.BlockSpec(memory_space=pltpu.VMEM)] * 3,
        out_specs=(pl.BlockSpec(memory_space=pltpu.VMEM),) * 3,
        compiler_params=pltpu.CompilerParams(vmem_limit_bytes=16 * 2**20),
        name="finish",
    )(*landed)
    return (
        jnp.swapaxes(key_cache, 0, 1)[None],
        jnp.swapaxes(value_cache, 0, 1)[None],
        reading.reshape(-1),
    )


def solution(mesh):
    placed = (P("sp", None), P(), P(), P(None, "tp"), P(None, "tp"), P(None, "tp"), P("sp", "tp"))
    return jax.shard_map(
        shards,
        mesh=mesh,
        in_specs=placed,
        out_specs=(P("sp", None, None, "tp"), P("sp", None, None, "tp"), P()),
        check_vma=False,
    )
```

```python
import functools

import jax
import jax.numpy as jnp
from jax import lax
from jax.experimental import pallas as pl
from jax.experimental.pallas import tpu as pltpu
from jax.sharding import PartitionSpec as P

HEAD_DIM = 128
MESH = pl.DeviceIdType.MESH


def norm_rows(rows, gain):
    wide = rows.astype(jnp.float32)
    inv_rms = lax.rsqrt(jnp.mean(wide * wide, axis=-1, keepdims=True) + 1e-06)
    return (wide * inv_rms * gain).astype(jnp.bfloat16)


def split_parts(wide, count):
    parts = []
    for _ in range(count):
        part = wide.astype(jnp.bfloat16).astype(jnp.float32)
        parts.append(part)
        wide = wide - part
    return jnp.concatenate(parts, axis=0).astype(jnp.bfloat16)


def fold_parts(rows, heads):
    total = rows[:heads]
    for first in range(heads, rows.shape[0], heads):
        total = total + rows[first : first + heads]
    return total


def kernel(
    n_sp, n_tp, chunks,
    x_hbm, next_hbm, gain_hbm, wk_hbm, wv_hbm, wq_hbm, offset_hbm,
    landed, read_out,
    x_in, normed, next_in, gain_in, wk, wv, wq, offset,
    outgoing, message, gathered, head_message, head_gathered,
    x_sem, load_sem, own_sem,
    b_ssem, b_rsem, m_ssem, m_rsem, h_ssem, h_rsem,
):
    me = lax.axis_index("sp")
    lane = lax.axis_index("tp")
    span, width = x_hbm.shape[0], wk_hbm.shape[1]
    heads = width // HEAD_DIM
    sub = span // n_sp
    rows = span // chunks

    load_gain, load_next, load_offset, load_key, load_query, load_value = [
        pltpu.make_async_copy(hbm, vmem, load_sem.at[n])
        for n, (hbm, vmem) in enumerate(
            [
                (gain_hbm, gain_in),
                (next_hbm, next_in),
                (offset_hbm, offset),
                (wk_hbm, wk),
                (wq_hbm, wq),
                (wv_hbm, wv),
            ]
        )
    ]
    x_loads = [
        pltpu.make_async_copy(
            x_hbm.at[pl.ds(c * rows, rows)], x_in.at[pl.ds(c * rows, rows)], x_sem.at[c]
        )
        for c in range(chunks)
    ]
    load_gain.start()
    for load in x_loads:
        load.start()
    load_key.start()
    load_next.start()
    load_offset.start()

    barrier = pltpu.get_barrier_semaphore()

    @pl.loop(1, n_sp)
    def _(step):
        pl.semaphore_signal(
            barrier, inc=1, device_id=(lax.rem(me + step, n_sp), lane), device_id_type=MESH
        )

    @pl.loop(1, n_tp)
    def _(step):
        pl.semaphore_signal(
            barrier, inc=1, device_id=(me, lax.rem(lane + step, n_tp)), device_id_type=MESH
        )

    load_gain.wait()
    gain = gain_in[...]
    step_rows = 16 if rows % 16 == 0 else rows
    for c in range(chunks):
        x_loads[c].wait()
        if c == 0:
            load_query.start()
        if c == chunks - 1:
            load_value.start()
        for first in range(c * rows, (c + 1) * rows, step_rows):
            normed[first : first + step_rows, :] = norm_rows(x_in[first : first + step_rows, :], gain)

    load_key.wait()
    wide_keys = jnp.dot(normed[...], wk[...], preferred_element_type=jnp.float32)
    keys = wide_keys.astype(jnp.bfloat16)

    load_next.wait()
    load_offset.wait()
    load_query.wait()
    next_row = next_in[...].astype(jnp.float32)
    next_row = jnp.concatenate([next_row[n : n + 1] for n in range(next_row.shape[0])], axis=1)
    query_normed = jnp.broadcast_to(norm_rows(next_row, gain), (16, x_hbm.shape[1]))
    query = jnp.dot(query_normed, wq[...], preferred_element_type=jnp.float32)
    row_ids = lax.broadcasted_iota(jnp.int32, query.shape, 0)
    head_ids = lax.broadcasted_iota(jnp.int32, query.shape, 1) // HEAD_DIM
    query = jnp.where(row_ids == head_ids, query, 0.0).astype(jnp.bfloat16)

    load_value.wait()
    logits = lax.dot_general(
        query, keys, (((1,), (1,)), ((), ())), preferred_element_type=jnp.float32
    )[:heads]
    logits = logits * HEAD_DIM ** (-0.5) + offset[...]
    tail = jnp.log1p(jnp.exp(-jnp.abs(logits)))
    log_breaks = -jnp.maximum(logits, 0.0) - tail
    later_than = (
        lax.broadcasted_iota(jnp.int32, (span, span), 0)
        > lax.broadcasted_iota(jnp.int32, (span, span), 1)
    )
    later_than = jnp.where(later_than, 1.0, 0.0).astype(jnp.bfloat16)
    inner = fold_parts(
        jnp.dot(split_parts(log_breaks, 3), later_than, preferred_element_type=jnp.float32), heads
    )
    block_total = jnp.sum(log_breaks, axis=1, keepdims=True)
    weights = jnp.exp(jnp.minimum(logits, 0.0) - tail + inner)

    wide_values = jnp.dot(normed[...], wv[...], preferred_element_type=jnp.float32)
    read = fold_parts(
        jnp.dot(
            split_parts(weights, 2),
            wide_values.astype(jnp.bfloat16),
            preferred_element_type=jnp.float32,
        ),
        heads,
    )
    for head in range(heads):
        message[head : head + 1, :] = read[head : head + 1, head * HEAD_DIM : (head + 1) * HEAD_DIM]
        message[heads + head : heads + head + 1, :] = jnp.broadcast_to(
            block_total[head : head + 1], (1, HEAD_DIM)
        )
    for slot in range(n_sp):
        outgoing[slot] = jnp.concatenate(
            [
                wide[slot * sub : (slot + 1) * sub, head * HEAD_DIM : (head + 1) * HEAD_DIM]
                for wide in (wide_keys, wide_values)
                for head in range(heads)
            ],
            axis=0,
        ).astype(jnp.bfloat16)

    pl.semaphore_wait(barrier, n_sp + n_tp - 2)

    def message_copy(step):
        return pltpu.make_async_remote_copy(
            src_ref=message, dst_ref=gathered.at[me],
            send_sem=m_ssem.at[step], recv_sem=m_rsem.at[step],
            device_id=(lax.rem(me + step, n_sp), lane), device_id_type=MESH,
        )

    def block_copy(step):
        to = lax.rem(me + step, n_sp)
        return pltpu.make_async_remote_copy(
            src_ref=outgoing.at[to], dst_ref=landed.at[me],
            send_sem=b_ssem.at[step], recv_sem=b_rsem.at[step],
            device_id=(to, lane), device_id_type=MESH,
        )

    @pl.loop(1, n_sp)
    def _(step):
        message_copy(step).start()

    @pl.loop(1, n_sp)
    def _(step):
        block_copy(step).start()

    own_message = pltpu.make_async_copy(message, gathered.at[me], own_sem.at[0])
    own_message.start()
    own_block = pltpu.make_async_copy(outgoing.at[me], landed.at[me], own_sem.at[1])
    own_block.start()
    own_message.wait()

    @pl.loop(1, n_sp)
    def _(step):
        message_copy(step).wait_recv()

    def add_block(step, carry):
        total, carried = carry
        block = gathered[n_sp - 1 - step]
        total = total + jnp.exp(carried) * block[:heads]
        return total, carried + block[heads : 2 * heads]

    zero = jnp.zeros((heads, HEAD_DIM), jnp.float32)
    total, _ = lax.fori_loop(0, n_sp, add_block, (zero, zero), unroll=n_sp <= 16)
    head_message[...] = total

    def head_copy(step):
        return pltpu.make_async_remote_copy(
            src_ref=head_message, dst_ref=head_gathered.at[lane],
            send_sem=h_ssem.at[step], recv_sem=h_rsem.at[step],
            device_id=(me, lax.rem(lane + step, n_tp)), device_id_type=MESH,
        )

    @pl.loop(1, n_tp)
    def _(step):
        head_copy(step).start()

    own_head = pltpu.make_async_copy(head_message, head_gathered.at[lane], own_sem.at[2])
    own_head.start()
    own_head.wait()

    @pl.loop(1, n_tp)
    def _(step):
        head_copy(step).wait_recv()

    read_out[...] = jnp.concatenate(
        [head_gathered[part] for part in range(n_tp)], axis=0
    ).astype(jnp.bfloat16)

    own_block.wait()

    @pl.loop(1, n_tp)
    def _(step):
        head_copy(step).wait_send()

    @pl.loop(1, n_sp)
    def _(step):
        message_copy(step).wait_send()
        block_copy(step).wait()


def finish(landed, read_in, k_out, v_out, read_out):
    sub, _, width = k_out.shape
    heads = width // HEAD_DIM
    for n, out in enumerate((k_out, v_out)):
        for head in range(heads):
            first = (n * heads + head) * sub
            piece = landed[...].astype(jnp.float32)[:, first : first + sub, :]
            out[:, :, head * HEAD_DIM : (head + 1) * HEAD_DIM] = jnp.swapaxes(
                piece, 0, 1
            ).astype(jnp.bfloat16)
    read_out[...] = read_in[...]


def shards(prompt_input, next_input, norm_gain, w_key, w_value, w_query, key_offset):
    span, depth = prompt_input.shape
    width = w_key.shape[1]
    heads = width // HEAD_DIM
    n_sp, n_tp = lax.axis_size("sp"), lax.axis_size("tp")
    sub = span // n_sp
    chunks = 3 if span % 48 == 0 else 1
    wide, narrow = jnp.float32, jnp.bfloat16
    blocks = (n_sp, 2 * heads * sub, HEAD_DIM)
    sems = pltpu.SemaphoreType.DMA
    landed = pl.pallas_call(
        functools.partial(kernel, n_sp, n_tp, chunks),
        out_shape=(
            jax.ShapeDtypeStruct(blocks, narrow),
            jax.ShapeDtypeStruct((n_tp * heads, HEAD_DIM), narrow),
        ),
        in_specs=[pl.BlockSpec(memory_space=pltpu.HBM)] * 7,
        out_specs=(pl.BlockSpec(memory_space=pltpu.VMEM),) * 2,
        scratch_shapes=[
            pltpu.VMEM((span, depth), narrow),
            pltpu.VMEM((span, depth), narrow),
            pltpu.VMEM((depth // HEAD_DIM, HEAD_DIM), narrow),
            pltpu.VMEM((1, depth), wide),
            pltpu.VMEM((depth, width), narrow),
            pltpu.VMEM((depth, width), narrow),
            pltpu.VMEM((depth, width), narrow),
            pltpu.VMEM((heads, span), wide),
            pltpu.VMEM(blocks, narrow),
            pltpu.VMEM((2 * heads, HEAD_DIM), wide),
            pltpu.VMEM((n_sp, 2 * heads, HEAD_DIM), wide),
            pltpu.VMEM((heads, HEAD_DIM), wide),
            pltpu.VMEM((n_tp, heads, HEAD_DIM), wide),
            sems((chunks,)),
            sems((6,)),
            sems((3,)),
            sems((n_sp,)),
            sems((n_sp,)),
            sems((n_sp,)),
            sems((n_sp,)),
            sems((n_tp,)),
            sems((n_tp,)),
        ],
        compiler_params=pltpu.CompilerParams(
            collective_id=0, has_side_effects=True, vmem_limit_bytes=16 * 2**20
        ),
        name="prefill",
    )(
        *[
            pltpu.with_memory_space_constraint(operand, pltpu.HBM)
            for operand in (
                prompt_input,
                next_input.reshape(-1, HEAD_DIM),
                norm_gain[None],
                w_key,
                w_value,
                w_query,
                key_offset.T,
            )
        ]
    )
    slotted = jax.ShapeDtypeStruct((sub, n_sp, width), narrow)
    key_cache, value_cache, reading = pl.pallas_call(
        finish,
        out_shape=(slotted, slotted, jax.ShapeDtypeStruct((n_tp * heads, HEAD_DIM), narrow)),
        in_specs=[pl.BlockSpec(memory_space=pltpu.VMEM)] * 2,
        out_specs=(pl.BlockSpec(memory_space=pltpu.VMEM),) * 3,
        compiler_params=pltpu.CompilerParams(vmem_limit_bytes=16 * 2**20),
        name="finish",
    )(*landed)
    return (
        jnp.swapaxes(key_cache, 0, 1)[None],
        jnp.swapaxes(value_cache, 0, 1)[None],
        reading.reshape(-1),
    )


def solution(mesh):
    placed = (P("sp", None), P(), P(), P(None, "tp"), P(None, "tp"), P(None, "tp"), P("sp", "tp"))
    return jax.shard_map(
        shards,
        mesh=mesh,
        in_specs=placed,
        out_specs=(P("sp", None, None, "tp"), P("sp", None, None, "tp"), P()),
        check_vma=False,
    )
```

```python
import functools

import jax
import jax.numpy as jnp
from jax import lax
from jax.experimental import pallas as pl
from jax.experimental.pallas import tpu as pltpu
from jax.sharding import PartitionSpec as P

HEAD_DIM = 128
MESH = pl.DeviceIdType.MESH


def norm_rows(rows, gain):
    wide = rows.astype(jnp.float32)
    inv_rms = lax.rsqrt(jnp.mean(wide * wide, axis=-1, keepdims=True) + 1e-06)
    return (wide * inv_rms * gain).astype(jnp.bfloat16)


def split_parts(wide, count):
    parts = []
    for _ in range(count):
        part = wide.astype(jnp.bfloat16).astype(jnp.float32)
        parts.append(part)
        wide = wide - part
    return jnp.concatenate(parts, axis=0).astype(jnp.bfloat16)


def fold_parts(rows, heads):
    total = rows[:heads]
    for first in range(heads, rows.shape[0], heads):
        total = total + rows[first : first + heads]
    return total


def kernel(
    n_sp, n_tp, chunks,
    x_hbm, next_hbm, gain_hbm, wk_hbm, wv_hbm, wq_hbm, offset_hbm,
    landed, read_out,
    x_in, normed, next_in, gain_in, wk, wv, wq, offset,
    outgoing, message, gathered, head_message, head_gathered,
    x_sem, load_sem, own_sem,
    b_ssem, b_rsem, m_ssem, m_rsem, h_ssem, h_rsem,
):
    me = lax.axis_index("sp")
    lane = lax.axis_index("tp")
    span, width = x_hbm.shape[0], wk_hbm.shape[1]
    heads = width // HEAD_DIM
    sub = span // n_sp
    rows = span // chunks

    load_gain, load_next, load_offset, load_key, load_query, load_value = [
        pltpu.make_async_copy(hbm, vmem, load_sem.at[n])
        for n, (hbm, vmem) in enumerate(
            [
                (gain_hbm, gain_in),
                (next_hbm, next_in),
                (offset_hbm, offset),
                (wk_hbm, wk),
                (wq_hbm, wq),
                (wv_hbm, wv),
            ]
        )
    ]
    x_loads = [
        pltpu.make_async_copy(
            x_hbm.at[pl.ds(c * rows, rows)], x_in.at[pl.ds(c * rows, rows)], x_sem.at[c]
        )
        for c in range(chunks)
    ]
    load_gain.start()
    for load in x_loads:
        load.start()
    load_key.start()
    load_next.start()
    load_offset.start()

    barrier = pltpu.get_barrier_semaphore()

    @pl.loop(1, n_sp)
    def _(step):
        pl.semaphore_signal(
            barrier, inc=1, device_id=(lax.rem(me + step, n_sp), lane), device_id_type=MESH
        )

    @pl.loop(1, n_tp)
    def _(step):
        pl.semaphore_signal(
            barrier, inc=1, device_id=(me, lax.rem(lane + step, n_tp)), device_id_type=MESH
        )

    load_gain.wait()
    gain = gain_in[...]
    step_rows = 16 if rows % 16 == 0 else rows
    for c in range(chunks):
        x_loads[c].wait()
        if c == 0:
            load_query.start()
        if c == chunks - 1:
            load_value.start()
        for first in range(c * rows, (c + 1) * rows, step_rows):
            normed[first : first + step_rows, :] = norm_rows(x_in[first : first + step_rows, :], gain)

    load_key.wait()
    wide_keys = jnp.dot(normed[...], wk[...], preferred_element_type=jnp.float32)
    keys = wide_keys.astype(jnp.bfloat16)

    load_next.wait()
    load_offset.wait()
    load_query.wait()
    next_row = next_in[...].astype(jnp.float32)
    next_row = jnp.concatenate([next_row[n : n + 1] for n in range(next_row.shape[0])], axis=1)
    query_normed = jnp.broadcast_to(norm_rows(next_row, gain), (16, x_hbm.shape[1]))
    query = jnp.dot(query_normed, wq[...], preferred_element_type=jnp.float32)
    row_ids = lax.broadcasted_iota(jnp.int32, query.shape, 0)
    head_ids = lax.broadcasted_iota(jnp.int32, query.shape, 1) // HEAD_DIM
    query = jnp.where(row_ids == head_ids, query, 0.0).astype(jnp.bfloat16)

    load_value.wait()
    logits = lax.dot_general(
        query, keys, (((1,), (1,)), ((), ())), preferred_element_type=jnp.float32
    )[:heads]
    logits = logits * HEAD_DIM ** (-0.5) + offset[...]
    tail = jnp.log1p(jnp.exp(-jnp.abs(logits)))
    log_breaks = -jnp.maximum(logits, 0.0) - tail
    later_than = (
        lax.broadcasted_iota(jnp.int32, (span, span), 0)
        > lax.broadcasted_iota(jnp.int32, (span, span), 1)
    )
    later_than = jnp.where(later_than, 1.0, 0.0).astype(jnp.bfloat16)
    inner = fold_parts(
        jnp.dot(split_parts(log_breaks, 3), later_than, preferred_element_type=jnp.float32), heads
    )
    block_total = jnp.sum(log_breaks, axis=1, keepdims=True)
    weights = jnp.exp(jnp.minimum(logits, 0.0) - tail + inner)

    wide_values = jnp.dot(normed[...], wv[...], preferred_element_type=jnp.float32)
    read = fold_parts(
        jnp.dot(
            split_parts(weights, 2),
            wide_values.astype(jnp.bfloat16),
            preferred_element_type=jnp.float32,
        ),
        heads,
    )
    for head in range(heads):
        message[head : head + 1, :] = read[head : head + 1, head * HEAD_DIM : (head + 1) * HEAD_DIM]
        message[heads + head : heads + head + 1, :] = jnp.broadcast_to(
            block_total[head : head + 1], (1, HEAD_DIM)
        )
    pl.semaphore_wait(barrier, n_sp + n_tp - 2)

    upper = me // ((n_sp + 1) // 2)

    def message_copy(step):
        return pltpu.make_async_remote_copy(
            src_ref=message, dst_ref=gathered.at[me],
            send_sem=m_ssem.at[step], recv_sem=m_rsem.at[step],
            device_id=(lax.rem(me + step, n_sp), lane), device_id_type=MESH,
        )

    def block_copy(step):
        to = lax.rem(me + step, n_sp)
        return pltpu.make_async_remote_copy(
            src_ref=outgoing.at[to], dst_ref=landed.at[me],
            send_sem=b_ssem.at[step], recv_sem=b_rsem.at[step],
            device_id=(to, lane), device_id_type=MESH,
        )

    @pl.loop(1, n_sp, unroll=n_sp <= 16)
    def _(near):
        message_copy(n_sp - near - upper * (n_sp - 2 * near)).start()

    for slot in range(n_sp):
        outgoing[slot] = jnp.concatenate(
            [
                wide[slot * sub : (slot + 1) * sub, head * HEAD_DIM : (head + 1) * HEAD_DIM]
                for wide in (wide_keys, wide_values)
                for head in range(heads)
            ],
            axis=0,
        ).astype(jnp.bfloat16)

    @pl.loop(1, n_sp)
    def _(near):
        block_copy(n_sp - near - upper * (n_sp - 2 * near)).start()

    own_message = pltpu.make_async_copy(message, gathered.at[me], own_sem.at[0])
    own_message.start()
    own_block = pltpu.make_async_copy(outgoing.at[me], landed.at[me], own_sem.at[1])
    own_block.start()
    own_message.wait()

    @pl.loop(1, n_sp)
    def _(step):
        message_copy(step).wait_recv()

    def add_block(step, carry):
        total, carried = carry
        block = gathered[n_sp - 1 - step]
        total = total + jnp.exp(carried) * block[:heads]
        return total, carried + block[heads : 2 * heads]

    zero = jnp.zeros((heads, HEAD_DIM), jnp.float32)
    total, _ = lax.fori_loop(0, n_sp, add_block, (zero, zero), unroll=n_sp <= 16)
    head_message[...] = total

    def head_copy(step):
        return pltpu.make_async_remote_copy(
            src_ref=head_message, dst_ref=head_gathered.at[lane],
            send_sem=h_ssem.at[step], recv_sem=h_rsem.at[step],
            device_id=(me, lax.rem(lane + step, n_tp)), device_id_type=MESH,
        )

    @pl.loop(1, n_tp, unroll=True)
    def _(step):
        head_copy(step).start()

    own_head = pltpu.make_async_copy(head_message, head_gathered.at[lane], own_sem.at[2])
    own_head.start()
    own_head.wait()

    @pl.loop(1, n_tp)
    def _(step):
        head_copy(step).wait_recv()

    read_out[...] = jnp.concatenate(
        [head_gathered[part] for part in range(n_tp)], axis=0
    ).astype(jnp.bfloat16)

    own_block.wait()

    @pl.loop(1, n_tp)
    def _(step):
        head_copy(step).wait_send()

    @pl.loop(1, n_sp)
    def _(step):
        message_copy(step).wait_send()
        block_copy(step).wait()


def finish(landed, read_in, k_out, v_out, read_out):
    sub, _, width = k_out.shape
    heads = width // HEAD_DIM
    for n, out in enumerate((k_out, v_out)):
        for head in range(heads):
            first = (n * heads + head) * sub
            piece = landed[...].astype(jnp.float32)[:, first : first + sub, :]
            out[:, :, head * HEAD_DIM : (head + 1) * HEAD_DIM] = jnp.swapaxes(
                piece, 0, 1
            ).astype(jnp.bfloat16)
    read_out[...] = read_in[...]


def shards(prompt_input, next_input, norm_gain, w_key, w_value, w_query, key_offset):
    span, depth = prompt_input.shape
    width = w_key.shape[1]
    heads = width // HEAD_DIM
    n_sp, n_tp = lax.axis_size("sp"), lax.axis_size("tp")
    sub = span // n_sp
    chunks = 3 if span % 48 == 0 else 1
    wide, narrow = jnp.float32, jnp.bfloat16
    blocks = (n_sp, 2 * heads * sub, HEAD_DIM)
    sems = pltpu.SemaphoreType.DMA
    landed = pl.pallas_call(
        functools.partial(kernel, n_sp, n_tp, chunks),
        out_shape=(
            jax.ShapeDtypeStruct(blocks, narrow),
            jax.ShapeDtypeStruct((n_tp * heads, HEAD_DIM), narrow),
        ),
        in_specs=[pl.BlockSpec(memory_space=pltpu.HBM)] * 7,
        out_specs=(pl.BlockSpec(memory_space=pltpu.VMEM),) * 2,
        scratch_shapes=[
            pltpu.VMEM((span, depth), narrow),
            pltpu.VMEM((span, depth), narrow),
            pltpu.VMEM((depth // HEAD_DIM, HEAD_DIM), narrow),
            pltpu.VMEM((1, depth), wide),
            pltpu.VMEM((depth, width), narrow),
            pltpu.VMEM((depth, width), narrow),
            pltpu.VMEM((depth, width), narrow),
            pltpu.VMEM((heads, span), wide),
            pltpu.VMEM(blocks, narrow),
            pltpu.VMEM((2 * heads, HEAD_DIM), wide),
            pltpu.VMEM((n_sp, 2 * heads, HEAD_DIM), wide),
            pltpu.VMEM((heads, HEAD_DIM), wide),
            pltpu.VMEM((n_tp, heads, HEAD_DIM), wide),
            sems((chunks,)),
            sems((6,)),
            sems((3,)),
            sems((n_sp,)),
            sems((n_sp,)),
            sems((n_sp,)),
            sems((n_sp,)),
            sems((n_tp,)),
            sems((n_tp,)),
        ],
        compiler_params=pltpu.CompilerParams(
            collective_id=0, has_side_effects=True, vmem_limit_bytes=16 * 2**20
        ),
        name="prefill",
    )(
        *[
            pltpu.with_memory_space_constraint(operand, pltpu.HBM)
            for operand in (
                prompt_input,
                next_input.reshape(-1, HEAD_DIM),
                norm_gain[None],
                w_key,
                w_value,
                w_query,
                key_offset.T,
            )
        ]
    )
    slotted = jax.ShapeDtypeStruct((sub, n_sp, width), narrow)
    key_cache, value_cache, reading = pl.pallas_call(
        finish,
        out_shape=(slotted, slotted, jax.ShapeDtypeStruct((n_tp * heads, HEAD_DIM), narrow)),
        in_specs=[pl.BlockSpec(memory_space=pltpu.VMEM)] * 2,
        out_specs=(pl.BlockSpec(memory_space=pltpu.VMEM),) * 3,
        compiler_params=pltpu.CompilerParams(vmem_limit_bytes=16 * 2**20),
        name="finish",
    )(*landed)
    return (
        jnp.swapaxes(key_cache, 0, 1)[None],
        jnp.swapaxes(value_cache, 0, 1)[None],
        reading.reshape(-1),
    )


def solution(mesh):
    placed = (P("sp", None), P(), P(), P(None, "tp"), P(None, "tp"), P(None, "tp"), P("sp", "tp"))
    return jax.shard_map(
        shards,
        mesh=mesh,
        in_specs=placed,
        out_specs=(P("sp", None, None, "tp"), P("sp", None, None, "tp"), P()),
        check_vma=False,
    )
```
